32 devices in a mesh: sp: 4 (over z), fs: 4 (over y, x), tp: 2 (over core).
Axes of the slice: x: 2, y: 2, z: 4, core: 2. Of those that a mesh axis runs over, the one named last changes fastest.
Arguments:
- stream: bfloat16 [4, 1024, 2048], P('fs', 'sp'), may hold values from -6 to 6
- norm_gain: bfloat16 [2048], replicated, may hold values from 0.099609375 to 1.8984375
- query_weight: bfloat16 [2048, 1024], P(None, 'tp'), may hold values from -0.125 to 0.125
- key_weight: bfloat16 [2048, 1024], P(None, 'tp'), may hold values from -0.125 to 0.125
- value_weight: bfloat16 [2048, 1024], P(None, 'tp'), may hold values from -0.125 to 0.125
- filter_input: bfloat16 [2048, 1024], P(None, 'tp'), may hold values from -0.125 to 0.125
- filter_gate: bfloat16 [2048, 1024], P(None, 'tp'), may hold values from -0.125 to 0.125
- score_offset: bfloat16 [4, 1024, 16], P('fs', 'sp', 'tp'), may hold values from -16 to 0
- head_gain: bfloat16 [1024], P('tp'), may hold values from 0.099609375 to 1.8984375
- filter_taps: bfloat16 [31, 1024], P(None, 'tp'), may hold values from -5 to 5
- channel_gain: bfloat16 [1024], P('tp'), may hold values from 0.099609375 to 1.8984375
- channel_shift: bfloat16 [1024], P('tp'), may hold values from -3 to 3
- attend_out: bfloat16 [1024, 2048], P('tp'), may hold values from -0.125 to 0.125
- filter_out: bfloat16 [1024, 2048], P('tp'), may hold values from -0.125 to 0.125
Outputs:
- mixed_out: bfloat16 [4, 1024, 2048], P('fs', ('sp', 'tp'))
- mass_log: float32 [4, 1024, 16], P('fs', 'sp', 'tp')
The draws below stay inside these ranges and needn't reach their ends.
All inputs are finite; a program needn't handle non-finite values.
Results may differ from the reference program's by a relative error of at most 0.015.
Values may be sent and summed in bfloat16 or wider, within the bound.
No kernel may reach another device: no remote copies, remote signals or barrier semaphores. Data moves between devices by JAX's collectives and lax.ppermute only.
A program may use at most 64 MiB of HBM per device.

```python
import math
import jax
import jax.numpy as jnp
from jax import lax

D = 2048
HEAD_COUNT = 16
HEAD_DIM = 64
CONV = 1024
KERNEL = 31
TOK_DEV = 256
ATTN = 1024
SEQUENCE_LENGTH = 1024
SEQUENCE_COUNT = 4


def draw_score_offset(key, part):
    key_collection = jax.random.split(jax.random.fold_in(key, 3), 4)
    slow_share = 0.5
    slowly = jax.random.bernoulli(key_collection[0], slow_share, (SEQUENCE_COUNT, 1, HEAD_COUNT))
    levels = jnp.where(slowly, math.log(0.15 / SEQUENCE_LENGTH), math.log(1.0 / 40.0))
    blocks = SEQUENCE_LENGTH // TOK_DEV
    shifts = jax.random.uniform(key_collection[1], (SEQUENCE_COUNT, blocks, 1, HEAD_COUNT), jnp.float32, -0.7, 0.7)
    shifts = jnp.broadcast_to(shifts, (SEQUENCE_COUNT, blocks, TOK_DEV, HEAD_COUNT)).reshape(SEQUENCE_COUNT, SEQUENCE_LENGTH, HEAD_COUNT)
    jitter = jax.random.uniform(key_collection[2], (SEQUENCE_COUNT, SEQUENCE_LENGTH, HEAD_COUNT), jnp.float32, -1.0, 1.0)
    break_fractions = jax.random.randint(key_collection[3], (SEQUENCE_COUNT, 4, 1, HEAD_COUNT), 0, SEQUENCE_LENGTH)
    slot_positions = jnp.arange(SEQUENCE_LENGTH, dtype=jnp.int32)[None, None, :, None]
    broken_weights = jnp.any(slot_positions == break_fractions, axis=1)
    values = jnp.where(broken_weights, -0.6 + 0.3 * jitter, levels + shifts + jitter)
    return values.astype(jnp.bfloat16)


def draw_filter_taps(key, part):
    entry_key, scale_key = jax.random.split(jax.random.fold_in(key, 7))
    channel = jnp.arange(CONV, dtype=jnp.float32) / CONV
    roughness = jax.random.uniform(scale_key, (1, CONV), jnp.float32, 0.7, 1.4)
    entries = jnp.clip(jax.random.normal(entry_key, (KERNEL, CONV), jnp.float32), -4.0, 4.0)
    scaling = 4.0 ** channel
    return (entries * scaling[None, :] * roughness / math.sqrt(KERNEL)).astype(jnp.bfloat16)


def block_scale(rng, shape, cuts, smallest, top_value):
    factor_of = 1.0
    for dim, shards_of in cuts:
        draws = jax.random.uniform(jax.random.fold_in(jax.random.fold_in(rng, 6), dim), (shards_of,), jnp.float32, smallest / len(cuts), top_value / len(cuts))
        factor_of = factor_of * jnp.repeat(jnp.exp(draws), shape[dim] // shards_of).reshape((-1,) + (1,) * (len(shape) - 1 - dim))
    return factor_of


def normal_values(own_key, dims, width, reach, shards=(), kind=jnp.bfloat16):
    array = width * jax.random.normal(own_key, dims, jnp.float32)
    if shards:
        array = array * block_scale(own_key, dims, shards, -0.22, 0.18)
    return jnp.clip(array, -reach, reach).astype(kind)


def setup_inputs(seed: int = 0) -> dict:
    key_of = jax.random.split(jax.random.key(seed), 15)
    return {
        "stream": normal_values(key_of[0], (SEQUENCE_COUNT, SEQUENCE_LENGTH, D), 1.0, 6.0, ((0, 4), (1, 4))),
        "norm_gain": jnp.clip(1.0 + 0.18 * jax.random.normal(key_of[1], (D,), jnp.float32), 0.099609375, 1.8984375).astype(jnp.bfloat16),
        "query_weight": normal_values(key_of[2], (D, ATTN), D ** -0.5, 0.125, ((1, 2),)),
        "key_weight": normal_values(key_of[3], (D, ATTN), D ** -0.5, 0.125, ((1, 2),)),
        "value_weight": normal_values(key_of[4], (D, ATTN), D ** -0.5, 0.125, ((1, 2),)),
        "filter_input": normal_values(key_of[5], (D, CONV), D ** -0.5, 0.125, ((1, 2),)),
        "filter_gate": normal_values(key_of[6], (D, CONV), D ** -0.5, 0.125, ((1, 2),)),
        "score_offset": draw_score_offset(jax.random.fold_in(key_of[14], 71), 0),
        "head_gain": jnp.clip(1.0 + 0.18 * jax.random.normal(key_of[8], (ATTN,), jnp.float32), 0.099609375, 1.8984375).astype(jnp.bfloat16),
        "filter_taps": draw_filter_taps(jax.random.fold_in(key_of[14], 71), 0),
        "channel_gain": jnp.clip(1.0 + 0.18 * jax.random.normal(key_of[10], (CONV,), jnp.float32), 0.099609375, 1.8984375).astype(jnp.bfloat16),
        "channel_shift": normal_values(key_of[11], (CONV,), 0.5, 3.0, ((0, 2),)),
        "attend_out": normal_values(key_of[12], (ATTN, D), (ATTN + CONV) ** -0.5, 0.125, ((0, 2),)),
        "filter_out": normal_values(key_of[13], (CONV, D), (ATTN + CONV) ** -0.5, 0.125, ((0, 2),)),
    }


rms_eps = 1e-06
norm_eps = 1e-05
mass_floor = 0.01

def attend_sequence(queries, keys_seq, values_seq, offsets):
    query_block = min(512, SEQUENCE_LENGTH)
    qfloat = queries.astype(jnp.float32).reshape(SEQUENCE_LENGTH, HEAD_COUNT, HEAD_DIM)
    kfloat = keys_seq.astype(jnp.float32).reshape(SEQUENCE_LENGTH, HEAD_COUNT, HEAD_DIM)
    vfloat = values_seq.astype(jnp.float32).reshape(SEQUENCE_LENGTH, HEAD_COUNT, HEAD_DIM)
    offsets_t = offsets.astype(jnp.float32).T
    key_pos = jnp.arange(SEQUENCE_LENGTH, dtype=jnp.int32)

    def one_block(block_index):
        first_row = (block_index * query_block).astype(jnp.int32)
        qpart = lax.dynamic_slice_in_dim(qfloat, first_row, query_block, 0)
        scores = jnp.einsum('thd,shd->hts', qpart, kfloat, precision=lax.Precision.HIGHEST) * HEAD_DIM ** (-0.5)
        scores = scores + offsets_t[:, None, :]
        query_pos = first_row + jnp.arange(query_block, dtype=jnp.int32)
        strict = key_pos[None, :] < query_pos[:, None]
        losing = jnp.where(strict[None], jax.nn.log_sigmoid(-scores), 0.0)
        beyond = lax.cumsum(losing, axis=2, reverse=True) - losing
        weights = jnp.where(strict[None], jnp.exp(jax.nn.log_sigmoid(scores) + beyond), 0.0)
        weight_mass = lax.optimization_barrier(jnp.sum(weights, axis=2))
        rounded = lax.optimization_barrier(weights.astype(jnp.bfloat16)).astype(jnp.float32)
        attended = jnp.einsum('hts,shd->thd', rounded, vfloat, precision=lax.Precision.HIGHEST)
        return (attended, weight_mass.T)
    attended, weight_mass = lax.map(one_block, jnp.arange(SEQUENCE_LENGTH // query_block, dtype=jnp.int32))
    return (attended.reshape(SEQUENCE_LENGTH, HEAD_COUNT, HEAD_DIM), weight_mass.reshape(SEQUENCE_LENGTH, HEAD_COUNT))

def reference(stream, norm_gain, query_weight, key_weight, value_weight, filter_input, filter_gate, score_offset, head_gain, filter_taps, channel_gain, channel_shift, attend_out, filter_out):
    xfloat = stream.astype(jnp.float32)
    normed = xfloat * lax.rsqrt(lax.optimization_barrier(jnp.mean(xfloat * xfloat, axis=-1, keepdims=True)) + rms_eps)
    normed = (normed * norm_gain.astype(jnp.float32)).astype(jnp.bfloat16)
    flat = normed.reshape(SEQUENCE_COUNT * SEQUENCE_LENGTH, D)

    def project(weight):
        return jnp.dot(flat, weight, preferred_element_type=jnp.float32).astype(jnp.bfloat16)
    queries = project(query_weight).reshape(SEQUENCE_COUNT, SEQUENCE_LENGTH, ATTN)
    keys_all = project(key_weight).reshape(SEQUENCE_COUNT, SEQUENCE_LENGTH, ATTN)
    values_all = project(value_weight).reshape(SEQUENCE_COUNT, SEQUENCE_LENGTH, ATTN)
    conv_values = project(filter_input)
    conv_gates = project(filter_gate)

    def per_sequence(seq_index):
        return attend_sequence(queries[seq_index], keys_all[seq_index], values_all[seq_index], score_offset[seq_index])
    attended, weight_mass = lax.map(per_sequence, jnp.arange(SEQUENCE_COUNT, dtype=jnp.int32))
    head_scale = lax.rsqrt(lax.optimization_barrier(jnp.mean(attended * attended, axis=-1, keepdims=True)) + rms_eps)
    heads_out = attended * head_scale * head_gain.astype(jnp.float32).reshape(HEAD_COUNT, HEAD_DIM)
    heads_out = heads_out.astype(jnp.bfloat16).reshape(SEQUENCE_COUNT * SEQUENCE_LENGTH, ATTN)
    mass_log = jnp.log(jnp.maximum(weight_mass, mass_floor))
    gated_rows = (conv_values.astype(jnp.float32) * jax.nn.sigmoid(conv_gates.astype(jnp.float32))).astype(jnp.bfloat16)
    gated_rows = gated_rows.reshape(SEQUENCE_COUNT, SEQUENCE_LENGTH, CONV)
    padded = jnp.pad(gated_rows.astype(jnp.float32), ((0, 0), (KERNEL - 1, 0), (0, 0)))
    tap_values = filter_taps.astype(jnp.float32)
    filtered = jnp.zeros((SEQUENCE_COUNT, SEQUENCE_LENGTH, CONV), jnp.float32)
    for tap_index in range(KERNEL):
        filtered = filtered + padded[:, tap_index:tap_index + SEQUENCE_LENGTH] * tap_values[tap_index]
    center = lax.optimization_barrier(jnp.mean(filtered, axis=-1, keepdims=True))
    deviation = filtered - center
    spread = lax.optimization_barrier(jnp.mean(deviation * deviation, axis=-1, keepdims=True))
    conv_out = jax.nn.silu(deviation * lax.rsqrt(spread + norm_eps) * channel_gain.astype(jnp.float32) + channel_shift.astype(jnp.float32)).astype(jnp.bfloat16)
    conv_out = conv_out.reshape(SEQUENCE_COUNT * SEQUENCE_LENGTH, CONV)
    mixed_out = jnp.dot(heads_out, attend_out, preferred_element_type=jnp.float32)
    mixed_out = mixed_out + jnp.dot(conv_out, filter_out, preferred_element_type=jnp.float32)
    return (mixed_out.astype(jnp.bfloat16).reshape(SEQUENCE_COUNT, SEQUENCE_LENGTH, D), mass_log)
```

```python
import functools
import math

import jax
import jax.numpy as jnp
from jax import lax
from jax.experimental import pallas as pl
from jax.experimental.pallas import tpu as pltpu
from jax.sharding import PartitionSpec as P

HEAD_DIM = 64
LANES = 128
PAIR = LANES // HEAD_DIM
PACK = 16
SUB = 8
LOG2E = math.log2(math.e)
TOP = 60.0
NEVER = -1e30

rms_eps = 1e-06
norm_eps = 1e-05
mass_floor = 0.01

f32 = jnp.float32
bf16 = jnp.bfloat16


def shifted(value, axis, steps):
    count = lax.axis_size(axis)
    first, last = (max(0, -steps), min(count, count - steps))
    return lax.ppermute(value, axis, [(source, source + steps) for source in range(first, last)])


def turned(value, axis, steps):
    count = lax.axis_size(axis)
    return lax.ppermute(value, axis, [(source, (source + steps) % count) for source in range(count)])


def params(mib=48):
    return pltpu.CompilerParams(vmem_limit_bytes=mib << 20)


def fixed(shape):
    return pl.BlockSpec(shape, lambda *step: (0,) * len(shape))


def cost(flops, size):
    return pl.CostEstimate(flops=int(flops), bytes_accessed=int(size), transcendentals=0)


def query_kernel(x_ref, gain_ref, w_ref, normed_ref, q_ref):
    @pl.when(pl.program_id(0) == 0)
    def _():
        x = x_ref[...].astype(f32)
        scale = lax.rsqrt(jnp.mean(x * x, axis=-1, keepdims=True) + rms_eps)
        normed_ref[...] = (x * scale * gain_ref[...].astype(f32)).astype(bf16)

    q = jnp.dot(normed_ref[...], w_ref[...], preferred_element_type=f32)
    q_ref[...] = (q * (LOG2E * HEAD_DIM ** (-0.5))).astype(bf16)


def project_queries(x, gain, weight):
    rows, width = x.shape
    cols = weight.shape[1]
    tile = min(256, cols)
    return pl.pallas_call(
        query_kernel,
        grid=(cols // tile,),
        in_specs=[fixed((rows, width)), fixed((1, width)), pl.BlockSpec((width, tile), lambda j: (0, j))],
        out_specs=[fixed((rows, width)), pl.BlockSpec((rows, tile), lambda j: (0, j))],
        out_shape=[jax.ShapeDtypeStruct((rows, width), bf16), jax.ShapeDtypeStruct((rows, cols), bf16)],
        compiler_params=params(),
        cost_estimate=cost(2 * rows * width * cols, 2 * width * (2 * rows + cols)),
        name="queries",
    )(x, gain, weight)


def ordering(rows):
    steps = rows // SUB
    place = lax.broadcasted_iota(jnp.int32, (rows, rows), 0)
    key = lax.broadcasted_iota(jnp.int32, (rows, rows), 1)
    return jnp.where((place % SUB) * steps + place // SUB == key, 1.0, 0.0).astype(bf16)


def block_kernel(half, x_ref, wk_ref, wv_ref, off_ref, out_ref, order_ref):
    rows = x_ref.shape[0]
    step = pl.program_id(0)

    @pl.when(step == 0)
    def _():
        order_ref[...] = ordering(rows)

    def put(weight):
        part = jnp.dot(x_ref[...], weight, preferred_element_type=f32).astype(bf16)
        out_ref[:rows, :] = jnp.dot(order_ref[...], part, preferred_element_type=f32).astype(bf16)

    @pl.when(step < half)
    def _():
        put(wk_ref[...])

    @pl.when(step >= half)
    def _():
        put(wv_ref[...])

    out_ref[rows:, :] = off_ref[...]


def project_block(normed, wk, wv, off_rows):
    rows, width = normed.shape
    cols = wk.shape[1]
    tile = min(256, cols)
    half = cols // tile
    extra = off_rows.shape[0]
    return pl.pallas_call(
        functools.partial(block_kernel, half),
        grid=(2 * half,),
        in_specs=[
            fixed((rows, width)),
            pl.BlockSpec((width, tile), lambda j: (0, jnp.minimum(j, half - 1))),
            pl.BlockSpec((width, tile), lambda j: (0, jnp.maximum(j - half, 0))),
            pl.BlockSpec((extra, tile), lambda j: (0, j)),
        ],
        out_specs=pl.BlockSpec((rows + extra, tile), lambda j: (0, j)),
        out_shape=jax.ShapeDtypeStruct((rows + extra, 2 * cols), bf16),
        scratch_shapes=[pltpu.VMEM((rows, rows), bf16)],
        compiler_params=params(),
        cost_estimate=cost(4 * rows * width * cols, 2 * width * (rows + 2 * cols)),
        name="keys_values",
    )(normed, wk, wv, off_rows)


def gate_kernel(x_ref, wi_ref, wg_ref, out_ref):
    values = jnp.dot(x_ref[...], wi_ref[...], preferred_element_type=f32).astype(bf16).astype(f32)
    gates = jnp.dot(x_ref[...], wg_ref[...], preferred_element_type=f32).astype(bf16).astype(f32)
    out_ref[...] = (values * (1.0 / (1.0 + jnp.exp(-gates)))).astype(bf16)


def project_gated(normed, wi, wg):
    rows, width = normed.shape
    cols = wi.shape[1]
    tile = min(256, cols)
    return pl.pallas_call(
        gate_kernel,
        grid=(cols // tile,),
        in_specs=[fixed((rows, width))] + [pl.BlockSpec((width, tile), lambda j: (0, j))] * 2,
        out_specs=pl.BlockSpec((rows, tile), lambda j: (0, j)),
        out_shape=jax.ShapeDtypeStruct((rows, cols), bf16),
        compiler_params=params(),
        cost_estimate=cost(4 * rows * width * cols, 2 * width * (rows + 2 * cols)),
        name="gated",
    )(normed, wi, wg)


def suffix_products(x):
    sub = lax.broadcasted_iota(jnp.int32, x.shape, 0)
    reach = 1
    while reach < SUB:
        x = x * jnp.where(sub < SUB - reach, pltpu.roll(x, SUB - reach, 0), 1.0)
        reach *= 2
    return x, jnp.where(sub < SUB - 1, pltpu.roll(x, SUB - 1, 0), 1.0)


def attend_kernel(causal, has_flag, packed, *refs):
    refs = list(refs)
    flag_ref = refs.pop(0) if has_flag else None
    q_ref = refs.pop(0)
    scores, weights, offs, vt = refs[-4:]
    outs = refs[-5:-4] if packed else refs[-6:-4]
    blocks = refs[: len(refs) - 4 - len(outs)]
    rows, width = q_ref.shape
    heads = width // HEAD_DIM
    steps = rows // SUB
    count = len(blocks)

    for b, block in enumerate(blocks):
        raw = block[rows : rows + PACK, :rows].astype(f32) * LOG2E
        if has_flag and b == count - 1:
            raw = jnp.where(flag_ref[0] > 0, raw, NEVER)
        raw = jnp.concatenate([raw, jnp.zeros((LANES - PACK, rows), f32)], axis=0)
        offs[b] = raw.T
        for p in range(width // LANES):
            v = block[:rows, width + p * LANES : width + (p + 1) * LANES]
            vt[b, p * LANES : (p + 1) * LANES, :] = v.T

    lane = lax.broadcasted_iota(jnp.int32, (rows, LANES), 1) // HEAD_DIM
    totals = []
    for h in range(heads):
        p, inside = h // PAIR, h % PAIR
        cols = slice(p * LANES, (p + 1) * LANES)
        q = jnp.where(lane == inside, q_ref[:, cols], jnp.zeros((), bf16))
        carry = jnp.ones((SUB, rows), f32)
        out = None
        for b, block in enumerate(blocks):
            scores[h % 2, b] = lax.dot_general(
                block[:rows, cols], q, (((1,), (1,)), ((), ())), preferred_element_type=f32
            )
            keep = jnp.ones((SUB, rows), f32)
            parts = [None] * steps
            for t in reversed(range(steps)):
                here = slice(t * SUB, (t + 1) * SUB)
                s = scores[h % 2, b, here, :] + offs[b, here, h : h + 1]
                e = jnp.exp2(jnp.minimum(s, TOP))
                if causal and b == 0:
                    key = lax.broadcasted_iota(jnp.int32, (SUB, rows), 0) * steps + t
                    e = jnp.where(key < lax.broadcasted_iota(jnp.int32, (SUB, rows), 1), e, 0.0)
                keep = keep * (1.0 / (1.0 + e))
                parts[t] = e * keep
            inclusive, exclusive = suffix_products(keep)
            after = exclusive * carry
            carry = carry * jnp.broadcast_to(inclusive[:1], (SUB, rows))
            for t in range(0, steps, 2):
                pair = jnp.concatenate([parts[t] * after, parts[t + 1] * after], axis=0)
                weights[h % 2, b, t * SUB : (t + 2) * SUB, :] = pair.astype(bf16)
            part = jnp.dot(
                vt[b, h * HEAD_DIM : (h + 1) * HEAD_DIM, :], weights[h % 2, b], preferred_element_type=f32
            )
            out = part if out is None else out + part
        totals.append(carry[:1])
        outs[0][h * HEAD_DIM : (h + 1) * HEAD_DIM, :] = out.astype(outs[0].dtype)

    rest = jnp.concatenate(totals, axis=0)
    if packed:
        mass = 1.0 - rest
        high = mass.astype(bf16)
        low = (mass - high.astype(f32)).astype(bf16)
        fill = outs[0].shape[0] - width - 2 * heads
        stats = [high.astype(f32), low.astype(f32)]
        if fill:
            stats.append(jnp.zeros((fill, rows), f32))
        outs[0][width:, :] = jnp.concatenate(stats, axis=0).astype(bf16)
    else:
        outs[1][...] = rest


def stat_rows(heads):
    return -(-2 * heads // PACK) * PACK


def attend(q, blocks, flag, causal, packed, name):
    rows, width = q.shape
    heads = width // HEAD_DIM
    count = len(blocks)
    if packed:
        out_shape = [jax.ShapeDtypeStruct((width + stat_rows(heads), rows), bf16)]
    else:
        out_shape = [jax.ShapeDtypeStruct((width, rows), f32), jax.ShapeDtypeStruct((heads, rows), f32)]
    whole = pl.BlockSpec(memory_space=pltpu.VMEM)
    args = ([] if flag is None else [flag]) + [q] + list(blocks)
    specs = ([] if flag is None else [pl.BlockSpec(memory_space=pltpu.SMEM)]) + [whole] * (1 + count)
    out = pl.pallas_call(
        functools.partial(attend_kernel, causal, flag is not None, packed),
        in_specs=specs,
        out_specs=[whole] * len(out_shape),
        out_shape=out_shape,
        scratch_shapes=[
            pltpu.VMEM((2, count, rows, rows), f32),
            pltpu.VMEM((2, count, rows, rows), bf16),
            pltpu.VMEM((count, rows, LANES), f32),
            pltpu.VMEM((count, width, rows), bf16),
        ],
        compiler_params=params(),
        cost_estimate=cost(600 * count * rows * rows * heads, 2 * rows * width * (2 + 2 * count)),
        name=name,
    )(*args)
    return out[0] if packed else out


def output_kernel(visits, me_ref, *refs):
    attA, restA, attC, restC = refs[:4]
    results = refs[4 : 4 + visits]
    gain_ref, conv_ref, wa_ref, wf_ref, out_ref, mass_ref, heads_ref, heads_bf = refs[4 + visits :]
    width, rows = attA.shape
    heads = width // HEAD_DIM
    shares = out_ref.shape[0]
    chunk = rows // shares

    @pl.when(pl.program_id(0) == 0)
    def _():
        rest = restA[...]
        scales = [rest]
        rest = rest * restC[...]
        for result in results:
            scales.append(rest)
            high = result[width : width + heads, :].astype(f32)
            low = result[width + heads : width + 2 * heads, :].astype(f32)
            rest = rest * (1.0 - (high + low))
        mass_ref[...] = jnp.log(jnp.maximum(1.0 - rest, mass_floor))
        for h in range(heads):
            mine = slice(h * HEAD_DIM, (h + 1) * HEAD_DIM)
            total = attA[mine, :] + scales[0][h : h + 1] * attC[mine, :]
            for result, scale in zip(results, scales[1:]):
                total = total + scale[h : h + 1] * result[mine, :].astype(f32)
            norm = lax.rsqrt(jnp.mean(total * total, axis=0, keepdims=True) + rms_eps)
            heads_ref[mine, :] = total * norm
        for p in range(width // LANES):
            cols = slice(p * LANES, (p + 1) * LANES)
            both = heads_ref[cols, :].T * gain_ref[:, cols].astype(f32)
            heads_bf[:, cols] = both.astype(bf16)

    me = me_ref[0]
    for t in range(shares):
        place = lax.rem(me + t, shares) * chunk
        mine = pl.ds(pl.multiple_of(place, chunk), chunk)
        got = jnp.dot(heads_bf[mine, :], wa_ref[...], preferred_element_type=f32)
        got = got + jnp.dot(conv_ref[mine, :], wf_ref[...], preferred_element_type=f32)
        out_ref[t] = got.astype(bf16)


def project_out(me, shares, attA, restA, attC, restC, results, gain, conv_out, wa, wf):
    width, rows = attA.shape
    heads = width // HEAD_DIM
    depth = wa.shape[1]
    tile = min(512, depth)

    return pl.pallas_call(
        functools.partial(output_kernel, len(results)),
        grid=(depth // tile,),
        in_specs=[pl.BlockSpec(memory_space=pltpu.SMEM)]
        + [fixed(a.shape) for a in (attA, restA, attC, restC, *results, gain, conv_out)]
        + [pl.BlockSpec((width, tile), lambda j: (0, j))] * 2,
        out_specs=[pl.BlockSpec((shares, rows // shares, tile), lambda j: (0, 0, j)), fixed((heads, rows))],
        out_shape=[
            jax.ShapeDtypeStruct((shares, rows // shares, depth), bf16),
            jax.ShapeDtypeStruct((heads, rows), f32),
        ],
        scratch_shapes=[pltpu.VMEM((width, rows), f32), pltpu.VMEM((rows, width), bf16)],
        compiler_params=params(),
        cost_estimate=cost(4 * rows * width * depth, 4 * width * depth),
        name="output",
    )(me, attA, restA, attC, restC, *results, gain, conv_out, wa, wf)


def local(
    stream,
    norm_gain,
    query_weight,
    key_weight,
    value_weight,
    filter_input,
    filter_gate,
    score_offset,
    head_gain,
    filter_taps,
    channel_gain,
    channel_shift,
    attend_out,
    filter_out,
):
    rows = stream.shape[1]
    width = query_weight.shape[1]
    heads = width // HEAD_DIM
    ring = lax.axis_size("sp")
    shares = lax.axis_size("tp")
    channels = filter_taps.shape[1] * shares

    normed, queries = project_queries(stream[0], norm_gain[None], query_weight)
    visiting = [shifted(queries, "sp", -2 * s) for s in range(1, (ring + 1) // 2)]

    off = score_offset[0].reshape(SUB, rows // SUB, heads).transpose(2, 1, 0).reshape(heads, rows)
    off = jnp.pad(off, ((0, -heads % PACK), (0, 2 * width - rows)))
    block = project_block(normed, key_weight, value_weight, off)
    block_before = shifted(block, "sp", 1)
    flag = (lax.axis_index("sp") > 0).astype(jnp.int32)[None]

    gated = project_gated(normed, filter_input, filter_gate)
    reach_back = filter_taps.shape[0] - 1
    earlier = shifted(gated[rows - reach_back :], "sp", 1)

    attA, restA = attend(queries, [block], None, True, False, "attend_own")
    results = []
    for s, visitor in enumerate(visiting):
        result = attend(visitor, [block, block_before], flag, False, True, "attend_visitor")
        results.append(shifted(result, "sp", 2 * (s + 1)))
    attC, restC = attend(queries, [block_before], flag, False, False, "attend_before")

    extended = jnp.concatenate([earlier, gated], axis=0).astype(f32)
    tap_values = filter_taps.astype(f32)
    filtered = jnp.zeros((rows, gated.shape[1]), f32)
    for tap_index in range(reach_back + 1):
        filtered = filtered + extended[tap_index : tap_index + rows] * tap_values[tap_index]
    here = filtered.shape[1]
    own_sum = jnp.sum(filtered, axis=-1)
    own_dev = filtered - (own_sum / here)[:, None]
    own_stats = jnp.stack([own_sum, jnp.sum(own_dev * own_dev, axis=-1)])
    stats = [own_stats] + [turned(own_stats, "tp", t) for t in range(1, shares)]
    center = sum(s[0] for s in stats) / channels
    spread = sum(s[1] + here * (s[0] / here - center) ** 2 for s in stats) / channels
    conv_out = jax.nn.silu(
        (filtered - center[:, None]) * lax.rsqrt(spread[:, None] + norm_eps) * channel_gain.astype(f32)
        + channel_shift.astype(f32)
    ).astype(bf16)

    me = lax.axis_index("tp").astype(jnp.int32)[None]
    out, mass = project_out(
        me, shares, attA, restA, attC, restC, results, head_gain[None], conv_out, attend_out, filter_out
    )
    total = out[0].astype(f32)
    for t in range(1, shares):
        total = total + turned(out[t], "tp", t).astype(f32)
    return (total.astype(bf16)[None], mass.T[None])


def solution(mesh):
    return jax.shard_map(
        local,
        mesh=mesh,
        in_specs=(
            P("fs", "sp", None),
            P(),
            P(None, "tp"),
            P(None, "tp"),
            P(None, "tp"),
            P(None, "tp"),
            P(None, "tp"),
            P("fs", "sp", "tp"),
            P("tp"),
            P(None, "tp"),
            P("tp"),
            P("tp"),
            P("tp", None),
            P("tp", None),
        ),
        out_specs=(P("fs", ("sp", "tp"), None), P("fs", "sp", "tp")),
        check_vma=False,
    )
```
